32 devices in a mesh: sp: 8 (over z, x), tp: 4 (over y, core).
Axes of the slice: x: 2, y: 2, z: 4, core: 2. Of those that a mesh axis runs over, the one named last changes fastest.
Arguments:
- residual: bfloat16 [1024, 2048], P(('sp', 'tp')), may hold values from -6 to 6
- query_first: bfloat16 [1024, 1024], P('sp', 'tp'), may hold values from -200 to 200
- key_first: bfloat16 [1024, 1024], P('sp', 'tp'), may hold values from -200 to 200
- query_second: bfloat16 [1024, 1024], P('sp', 'tp'), may hold values from -200 to 200
- key_second: bfloat16 [1024, 1024], P('sp', 'tp'), may hold values from -200 to 200
- values: bfloat16 [1024, 2048], P('sp', 'tp'), may hold values from -6 to 6
- lambda_weight: float32 [16], P('tp'), may hold values from 0.3 to 0.8
- head_gain: float32 [128], replicated, may hold values from 0.1 to 1.9
- out_weight: bfloat16 [2048, 2048], P('sp', 'tp'), may hold values from -0.125 to 0.125
- norm_gain: float32 [2048], replicated, may hold values from 0.1 to 1.9
- gate_weight: bfloat16 [2048, 5632], P(None, 'tp'), may hold values from -0.125 to 0.125
- up_weight: bfloat16 [2048, 5632], P(None, 'tp'), may hold values from -0.125 to 0.125
- down_weight: bfloat16 [2048, 5632], P('sp', 'tp'), may hold values from -0.078125 to 0.078125
Outputs:
- layer_out: bfloat16 [1024, 2048], P(('sp', 'tp'))
The draws below stay inside these ranges and needn't reach their ends.
All inputs are finite; a program needn't handle non-finite values.
Results may differ from the reference program's by a relative error of at most 0.017.
Values may be sent and summed in bfloat16 or wider, within the bound.
A program may use at most 128 MiB of HBM per device.

```python
import jax
import jax.numpy as jnp
from jax import lax

D = 2048
HEADS = 16
HD = 64
VD = 128
FF = 5632
TOKENS = 1024
N_TP = 4


def plant_pair(key, which):
    spread = 1.32
    key_rows = jax.random.normal(jax.random.fold_in(key, 101 + which), (TOKENS, HEADS * HD), jnp.float32) * spread
    key_rows = jnp.clip(key_rows, -6.0 * spread, 6.0 * spread)
    queries = jax.random.normal(jax.random.fold_in(key, 201 + which), (TOKENS, HEADS * HD), jnp.float32) * spread
    queries = jnp.clip(queries, -6.0 * spread, 6.0 * spread)
    return (queries, key_rows)


def draw_query_first(key, part):
    return plant_pair(key, 0)[0].astype(jnp.bfloat16)


def draw_key_first(key, part):
    return plant_pair(key, 0)[1].astype(jnp.bfloat16)


def draw_query_second(key, part):
    return plant_pair(key, 1)[0].astype(jnp.bfloat16)


def draw_key_second(key, part):
    return plant_pair(key, 1)[1].astype(jnp.bfloat16)


def shard_levels(rng, shape, cuts, low, high):
    def one(axis_at, blocks):
        steps = jax.random.uniform(jax.random.fold_in(jax.random.fold_in(rng, 6), axis_at), (blocks,), jnp.float32, low / len(cuts), high / len(cuts))
        return jnp.repeat(jnp.exp(steps), shape[axis_at] // blocks).reshape((-1,) + (1,) * (len(shape) - axis_at - 1))

    level = one(*cuts[0])
    for cut in cuts[1:]:
        level = level * one(*cut)
    return level


def normal_values(stream_key, extent, deviation, reach, cuts=(), held_as=jnp.bfloat16):
    loudness = shard_levels(stream_key, extent, cuts, -0.22, 0.18) if cuts else 1.0
    values = jax.random.normal(stream_key, extent, jnp.float32) * deviation * loudness
    return jnp.minimum(jnp.maximum(values, -reach), reach).astype(held_as)


def setup_inputs(seed: int = 0) -> dict:
    arg_keys = jax.random.split(jax.random.key(seed), 14)
    residual = normal_values(arg_keys[0], (TOKENS, D), 1.0, 6.0, ((0, 32),))
    query_first = draw_query_first(jax.random.fold_in(arg_keys[13], 71), 0)
    key_first = draw_key_first(jax.random.fold_in(arg_keys[13], 71), 0)
    query_second = draw_query_second(jax.random.fold_in(arg_keys[13], 71), 0)
    key_second = draw_key_second(jax.random.fold_in(arg_keys[13], 71), 0)
    values = normal_values(arg_keys[5], (TOKENS, HEADS * VD), 1.0, 6.0, ((0, 8), (1, 4)))
    lambda_weight = jnp.clip(0.3 + 0.5 * jax.random.uniform(arg_keys[6], (HEADS,), jnp.float32) ** shard_levels(arg_keys[6], (HEADS,), ((0, 4),), -0.2, 0.2), 0.3, 0.8)
    head_gain = jnp.clip(1.0 + 0.18 * jax.random.normal(arg_keys[7], (VD,), jnp.float32), 0.1, 1.9)
    out_weight = normal_values(arg_keys[8], (D, HEADS * VD), (HEADS * VD) ** -0.5, 0.125, ((0, 8), (1, 4)))
    norm_gain = jnp.clip(1.0 + 0.18 * jax.random.normal(arg_keys[9], (D,), jnp.float32), 0.1, 1.9)
    gate_weight = normal_values(arg_keys[10], (D, FF), D ** -0.5, 0.125, ((1, 4),))
    up_weight = normal_values(arg_keys[11], (D, FF), D ** -0.5, 0.125, ((1, 4),))
    down_weight = normal_values(arg_keys[12], (D, FF), FF ** -0.5, 0.078125, ((0, 8), (1, 4)))
    return {"residual": residual, "query_first": query_first, "key_first": key_first, "query_second": query_second, "key_second": key_second, "values": values, "lambda_weight": lambda_weight, "head_gain": head_gain, "out_weight": out_weight, "norm_gain": norm_gain, "gate_weight": gate_weight, "up_weight": up_weight, "down_weight": down_weight}


epsilon = 1e-06

def one_map(queries, key_rows, value_rows):
    scores = jnp.dot(queries, key_rows.T, preferred_element_type=jnp.float32) * queries.shape[-1] ** (-0.5)
    shifted = jnp.exp(scores - lax.optimization_barrier(jnp.max(scores, axis=-1, keepdims=True)))
    totals = lax.optimization_barrier(jnp.sum(shifted, axis=-1, keepdims=True))
    product = jnp.dot(shifted.astype(jnp.bfloat16), value_rows, preferred_element_type=jnp.float32)
    return product / totals

def attend_head(inputs, head_gain):
    query_one, key_one, query_two, key_two, value_rows, weight = inputs
    first_map = one_map(query_one, key_one, value_rows)
    second_map = one_map(query_two, key_two, value_rows)
    difference = first_map - weight * second_map
    scaled = difference * lax.rsqrt(lax.optimization_barrier(jnp.mean(difference * difference, axis=-1, keepdims=True)) + epsilon)
    return (scaled * head_gain).astype(jnp.bfloat16)

def reference(residual, query_first, key_first, query_second, key_second, values, lambda_weight, head_gain, out_weight, norm_gain, gate_weight, up_weight, down_weight):
    length = query_first.shape[0]

    def split_heads(array, entries):
        return array.reshape(length, HEADS, entries).transpose(1, 0, 2)
    stacked = (split_heads(query_first, HD), split_heads(key_first, HD), split_heads(query_second, HD), split_heads(key_second, HD), split_heads(values, VD), lambda_weight)
    heads_out = lax.map(lambda inputs: attend_head(inputs, head_gain), stacked)
    attended = heads_out.transpose(1, 0, 2).reshape(length, HEADS * VD)
    group_width = HEADS * VD // N_TP
    projected = jnp.zeros((length, D), jnp.float32)
    for member in range(N_TP):
        columns = slice(member * group_width, (member + 1) * group_width)
        partial_value = lax.dot_general(attended[:, columns], out_weight[:, columns], (((1,), (1,)), ((), ())), preferred_element_type=jnp.float32)
        projected = projected + lax.optimization_barrier(partial_value.astype(jnp.bfloat16)).astype(jnp.float32)
    after_attention = (residual.astype(jnp.float32) + projected).astype(jnp.bfloat16)
    stream = after_attention.astype(jnp.float32)
    normed = (stream * lax.rsqrt(lax.optimization_barrier(jnp.mean(stream * stream, axis=-1, keepdims=True)) + epsilon) * norm_gain).astype(jnp.bfloat16)
    hidden_width = FF // N_TP
    feed_sum = jnp.zeros((length, D), jnp.float32)
    for member in range(N_TP):
        columns = slice(member * hidden_width, (member + 1) * hidden_width)
        gate_part = jnp.dot(normed, gate_weight[:, columns], preferred_element_type=jnp.float32)
        up_part = jnp.dot(normed, up_weight[:, columns], preferred_element_type=jnp.float32)
        hidden = (jax.nn.silu(gate_part) * up_part).astype(jnp.bfloat16)
        partial_value = lax.dot_general(hidden, down_weight[:, columns], (((1,), (1,)), ((), ())), preferred_element_type=jnp.float32)
        feed_sum = feed_sum + lax.optimization_barrier(partial_value.astype(jnp.bfloat16)).astype(jnp.float32)
    return (stream + feed_sum).astype(jnp.bfloat16)
```

```python
import functools

import jax
import jax.numpy as jnp
from jax import lax
from jax.experimental import pallas as pl
from jax.experimental.pallas import tpu as pltpu
from jax.sharding import PartitionSpec as P

epsilon = 1e-06
ROWS_ROWS = (((1,), (1,)), ((), ()))


def split_sp(size):
    inner = 1
    while (2 * inner) * (2 * inner) <= size:
        inner *= 2
    return size // inner, inner


def kernel(
    Z,
    X,
    T,
    heads,
    residual,
    q_one,
    k_one,
    q_two,
    k_two,
    values,
    lam,
    head_gain,
    out_weight,
    norm_gain,
    gate_weight,
    up_weight,
    down_weight,
    result,
    kv,
    outw,
    downw,
    gate,
    up,
    attended,
    part,
    rec_one,
    after,
    normed,
    hidden,
    hidden_other,
    part_two,
    rec_two,
    local_sem,
    send_sem,
    recv_sem,
):
    f32, bf16 = jnp.float32, jnp.bfloat16
    s = lax.axis_index("sp")
    t = lax.axis_index("tp")
    z, x = s // X, s % X
    parity = z % 2
    zpair = z + 1 - 2 * parity
    spair = zpair * X + x
    tokens = q_one.shape[0]
    piece = tokens // T
    kw = k_one.shape[1]
    vw = values.shape[1]
    model = result.shape[1]
    group = X * down_weight.shape[0]

    def at_z(d):
        return (z + d) % Z

    def from_z(d):
        return (z - d + Z) % Z

    def at_x(d):
        return (x + d) % X

    def from_x(d):
        return (x - d + X) % X

    def at_t(d):
        return (t + d) % T

    def from_t(d):
        return (t - d + T) % T

    barrier = pltpu.get_barrier_semaphore()
    peers = [(at_z(d) * X + x, t) for d in range(1, Z)]
    peers += [(z * X + at_x(d), t) for d in range(1, X)]
    peers += [(s, at_t(d)) for d in range(1, T)]
    peers += [(spair, at_t(d)) for d in range(1, T)]
    for sp_at, tp_at in peers:
        pl.semaphore_signal(
            barrier, inc=1, device_id={"sp": sp_at, "tp": tp_at},
            device_id_type=pl.DeviceIdType.MESH,
        )

    locals_ = [
        pltpu.make_async_copy(k_one, kv.at[s, :, pl.ds(0, kw)], local_sem.at[0]),
        pltpu.make_async_copy(k_two, kv.at[s, :, pl.ds(kw, kw)], local_sem.at[1]),
        pltpu.make_async_copy(values, kv.at[s, :, pl.ds(2 * kw, vw)], local_sem.at[2]),
        pltpu.make_async_copy(out_weight, outw.at[s], local_sem.at[3]),
        pltpu.make_async_copy(down_weight, downw.at[z // 2, x], local_sem.at[4]),
        pltpu.make_async_copy(gate_weight, gate, local_sem.at[5]),
        pltpu.make_async_copy(up_weight, up, local_sem.at[6]),
    ]
    for copy in locals_:
        copy.start()

    names = {}
    sent = []

    def slot(name):
        return names.setdefault(name, len(names))

    def send(src, dst, name, sp_at, tp_at):
        k = slot(name)
        copy = pltpu.make_async_remote_copy(
            src_ref=src, dst_ref=dst, send_sem=send_sem.at[k], recv_sem=recv_sem.at[k],
            device_id={"sp": sp_at, "tp": tp_at}, device_id_type=pl.DeviceIdType.MESH,
        )
        copy.start()
        sent.append(copy)

    def arrive(ref, name):
        k = slot(name)
        pltpu.make_async_remote_copy(
            src_ref=ref, dst_ref=ref, send_sem=send_sem.at[k], recv_sem=recv_sem.at[k],
            device_id={"sp": s, "tp": t}, device_id_type=pl.DeviceIdType.MESH,
        ).wait_recv()

    def by_s(buffer):
        return lambda zz, xx: buffer.at[zz * X + xx]

    def down_at(zz, xx):
        return downw.at[zz // 2, xx]

    kv_at, out_at = by_s(kv), by_s(outw)

    def send_z(kind, ref, d):
        send(ref(z, x), ref(z, x), (kind, "z", d), at_z(d) * X + x, t)

    def wait_z(kind, ref, d):
        arrive(ref(from_z(d), x), (kind, "z", d))

    def forward_x(kind, ref, d):
        for dx in range(1, X):
            block = ref(from_z(d), x)
            send(block, block, (kind, "x", d, dx), z * X + at_x(dx), t)

    def wait_x(kind, ref, d):
        for dx in range(1, X):
            arrive(ref(from_z(d), from_x(dx)), (kind, "x", d, dx))

    for copy in locals_[:3]:
        copy.wait()
    pl.semaphore_wait(barrier, len(peers))
    for d in range(1, Z):
        send_z("kv", kv_at, d)
    forward_x("kv", kv_at, 0)
    locals_[3].wait()
    for d in range(1, Z):
        send_z("out", out_at, d)
    locals_[4].wait()
    for d in range(2, Z, 2):
        send_z("down", down_at, d)
    for d in range(1, Z):
        wait_z("kv", kv_at, d)
        forward_x("kv", kv_at, d)
    forward_x("out", out_at, 0)
    for d in range(Z):
        wait_x("kv", kv_at, d)

    head_size = q_one.shape[1] // heads
    value_size = vw // heads
    per = 128 // head_size
    scale = head_size ** (-0.5)
    source_count = kv.shape[0]
    block_count = max(1, (source_count * tokens) // 1024)
    block_sources = source_count // block_count
    block_keys = block_sources * tokens
    lanes = lax.broadcasted_iota(jnp.int32, (1, per * head_size), 1) // head_size

    def map_outputs(q_ref, base, first):
        width = per * head_size
        q = q_ref[:, first * head_size : first * head_size + width]
        stacked = jnp.concatenate(
            [jnp.where(lanes == i, q, jnp.zeros_like(q)) for i in range(per)], axis=0
        )

        def block(b, state):
            rows = pl.ds(b * block_sources, block_sources)
            keys = kv[rows, :, base + first * head_size : base + first * head_size + width]
            scores = lax.dot_general(
                stacked, keys.reshape(block_keys, width), ROWS_ROWS, preferred_element_type=f32
            ) * scale
            newest = jnp.max(scores, axis=1, keepdims=True)
            if state is not None:
                newest = jnp.maximum(newest, state[0])
            shifted = jnp.exp(scores - newest)
            totals = jnp.sum(shifted, axis=1, keepdims=True)
            rounded = shifted.astype(bf16)
            products = []
            for i in range(per):
                start = 2 * kw + (first + i) * value_size
                v = kv[rows, :, start : start + value_size].reshape(block_keys, value_size)
                products.append(
                    jnp.dot(
                        rounded[i * tokens : (i + 1) * tokens], v, preferred_element_type=f32
                    )
                )
            product = jnp.concatenate(products, axis=0)
            if state is not None:
                factor = jnp.exp(state[0] - newest)
                totals = totals + state[1] * factor
                product = product + state[2] * factor
            return newest, totals, product

        if block_count == 1:
            state = block(0, None)
        else:
            state = lax.fori_loop(
                0,
                block_count,
                block,
                (
                    jnp.full((per * tokens, 1), -jnp.inf, f32),
                    jnp.zeros((per * tokens, 1), f32),
                    jnp.zeros((per * tokens, value_size), f32),
                ),
            )
        return state[2] / state[1]

    for first in range(0, heads, per):
        one = map_outputs(q_one, 0, first)
        two = map_outputs(q_two, kw, first)
        for i in range(per):
            rows = slice(i * tokens, (i + 1) * tokens)
            difference = one[rows] - lam[first + i] * two[rows]
            scaled = difference * lax.rsqrt(
                jnp.mean(difference * difference, axis=1, keepdims=True) + epsilon
            )
            start = (first + i) * value_size
            attended[:, start : start + value_size] = (scaled * head_gain[...]).astype(bf16)

    for d in range(1, Z):
        wait_z("out", out_at, d)
        forward_x("out", out_at, d)
    forward_x("down", down_at, 0)
    for d in range(Z):
        wait_x("out", out_at, d)

    rows_out = out_weight.shape[0]
    chunk = min(512, model)
    for c in range(0, model, chunk):
        cols = slice(c, c + chunk)
        weight = outw[c // rows_out : (c + chunk) // rows_out].reshape(chunk, vw)
        product = lax.dot_general(
            attended[...], weight, ROWS_ROWS, preferred_element_type=f32
        ).astype(bf16)
        part[:, :, cols] = product.reshape(T, piece, chunk)
        for d in range(1, T):
            send(
                part.at[at_t(d), :, pl.ds(c, chunk)],
                rec_one.at[t, :, pl.ds(c, chunk)],
                ("one", c, d), s, at_t(d),
            )
    rec_one[t] = part[t]
    for c in range(0, model, chunk):
        for d in range(1, T):
            arrive(rec_one.at[from_t(d), :, pl.ds(c, chunk)], ("one", c, d))
    summed = rec_one[0].astype(f32)
    for i in range(1, T):
        summed = summed + rec_one[i].astype(f32)
    stream = (residual[...].astype(f32) + summed).astype(bf16).astype(f32)
    after[...] = stream
    scaled = stream * lax.rsqrt(jnp.mean(stream * stream, axis=1, keepdims=True) + epsilon)
    normed[t] = (scaled * norm_gain[...]).astype(bf16)
    for d in range(1, T):
        send(normed.at[t], normed.at[t], ("norm", d), s, at_t(d))
    locals_[5].wait()
    locals_[6].wait()
    for d in range(1, T):
        arrive(normed.at[from_t(d)], ("norm", d))

    width = hidden.shape[1]
    spans = [(c, min(512, width - c)) for c in range(0, width, 512)]
    rows_in = normed[...].reshape(tokens, model)
    for c, n in spans:
        gate_part = jnp.dot(rows_in, gate[:, c : c + n], preferred_element_type=f32)
        up_part = jnp.dot(rows_in, up[:, c : c + n], preferred_element_type=f32)
        hidden[:, c : c + n] = (gate_part / (1.0 + jnp.exp(-gate_part)) * up_part).astype(bf16)
        send(
            hidden.at[:, pl.ds(c, n)], hidden_other.at[:, pl.ds(c, n)], ("hid", c), spair, t
        )
    for d in range(2, Z, 2):
        wait_z("down", down_at, d)
        forward_x("down", down_at, d)
    for d in range(0, Z, 2):
        wait_x("down", down_at, d)

    def project(which, source, sp_at, first_step):
        for g in range(Z // 2):
            cols = slice(g * group, (g + 1) * group)
            product = lax.dot_general(
                source[...], downw[g].reshape(group, width), ROWS_ROWS,
                preferred_element_type=f32,
            ).astype(bf16)
            part_two[which, :, :, cols] = product.reshape(T, piece, group)
            for d in range(first_step, T):
                send(
                    part_two.at[which, at_t(d), :, pl.ds(g * group, group)],
                    rec_two.at[parity, t, :, pl.ds(g * group, group)],
                    ("two", which, g, d), sp_at, at_t(d),
                )

    for c, n in spans:
        arrive(hidden_other.at[:, pl.ds(c, n)], ("hid", c))
    project(1, hidden_other, spair, 0)
    project(0, hidden, s, 1)
    rec_two[parity, t] = part_two[0, t]
    for g in range(Z // 2):
        for d in range(1, T):
            arrive(
                rec_two.at[parity, from_t(d), :, pl.ds(g * group, group)], ("two", 0, g, d)
            )
        for d in range(T):
            arrive(
                rec_two.at[1 - parity, from_t(d), :, pl.ds(g * group, group)], ("two", 1, g, d)
            )
    for side in range(2):
        for g in range(Z // 2):
            start = (2 * g + side) * group
            total = rec_two[side, 0, :, g * group : (g + 1) * group].astype(f32)
            for i in range(1, T):
                total = total + rec_two[side, i, :, g * group : (g + 1) * group].astype(f32)
            result[:, start : start + group] = (
                after[:, start : start + group] + total
            ).astype(bf16)
    for copy in sent:
        copy.wait_send()


def local(Z, X, T, *arrays):
    (residual, q_one, k_one, q_two, k_two, values, lam, head_gain, out_weight, norm_gain,
     gate_weight, up_weight, down_weight) = arrays
    sp = Z * X
    bf16 = jnp.bfloat16
    tokens, kw = k_one.shape
    vw = values.shape[1]
    piece, model = residual.shape
    width = gate_weight.shape[1]
    rows_down = down_weight.shape[0]
    half = model // 2
    vmem = pl.BlockSpec(memory_space=pltpu.VMEM)
    anywhere = pl.BlockSpec(memory_space=pl.ANY)
    smem = pl.BlockSpec(memory_space=pltpu.SMEM)
    semaphores = 2 * (Z + Z * X) + Z + Z * X + 64
    return pl.pallas_call(
        functools.partial(kernel, Z, X, T, lam.shape[0]),
        out_shape=jax.ShapeDtypeStruct((piece, model), bf16),
        in_specs=[
            vmem, vmem, anywhere, vmem, anywhere, anywhere, smem, vmem, anywhere, vmem,
            anywhere, anywhere, anywhere,
        ],
        out_specs=vmem,
        scratch_shapes=[
            pltpu.VMEM((sp, tokens, 2 * kw + vw), bf16),
            pltpu.VMEM((sp, out_weight.shape[0], vw), bf16),
            pltpu.VMEM((Z // 2, X, rows_down, width), bf16),
            pltpu.VMEM(gate_weight.shape, bf16),
            pltpu.VMEM(up_weight.shape, bf16),
            pltpu.VMEM((tokens, vw), bf16),
            pltpu.VMEM((T, piece, model), bf16),
            pltpu.VMEM((T, piece, model), bf16),
            pltpu.VMEM((piece, model), jnp.float32),
            pltpu.VMEM((T, piece, model), bf16),
            pltpu.VMEM((tokens, width), bf16),
            pltpu.VMEM((tokens, width), bf16),
            pltpu.VMEM((2, T, piece, half), bf16),
            pltpu.VMEM((2, T, piece, half), bf16),
            pltpu.SemaphoreType.DMA((7,)),
            pltpu.SemaphoreType.DMA((semaphores,)),
            pltpu.SemaphoreType.DMA((semaphores,)),
        ],
        compiler_params=pltpu.CompilerParams(
            collective_id=0, has_side_effects=True, vmem_limit_bytes=60 * 1024 * 1024
        ),
    )(
        residual, q_one, k_one, q_two, k_two, values, lam, head_gain.reshape(1, -1), out_weight,
        norm_gain.reshape(1, -1), gate_weight, up_weight, down_weight,
    )


def solution(mesh):
    Z, X = split_sp(mesh.shape["sp"])
    return jax.shard_map(
        functools.partial(local, Z, X, mesh.shape["tp"]),
        mesh=mesh,
        in_specs=(
            P(("sp", "tp"), None),
            P("sp", "tp"),
            P("sp", "tp"),
            P("sp", "tp"),
            P("sp", "tp"),
            P("sp", "tp"),
            P("tp"),
            P(),
            P("sp", "tp"),
            P(),
            P(None, "tp"),
            P(None, "tp"),
            P("sp", "tp"),
        ),
        out_specs=P(("sp", "tp"), None),
        check_vma=False,
    )
```

```python
import functools

import jax
import jax.numpy as jnp
from jax import lax
from jax.experimental import pallas as pl
from jax.experimental.pallas import tpu as pltpu
from jax.sharding import PartitionSpec as P

epsilon = 1e-06
ROWS_ROWS = (((1,), (1,)), ((), ()))


def split_sp(size):
    inner = 1
    while (2 * inner) * (2 * inner) <= size:
        inner *= 2
    return size // inner, inner


def kernel(
    Z,
    X,
    T,
    C,
    heads,
    residual,
    q_one,
    k_one,
    q_two,
    k_two,
    values,
    lam,
    head_gain,
    out_weight,
    norm_gain,
    gate_weight,
    up_weight,
    down_weight,
    result,
    queries,
    queries_out,
    kv,
    kv_out,
    outw,
    downw,
    gate,
    up,
    attended,
    part_one,
    rec_one,
    after,
    normed,
    hidden,
    part_two,
    rec_two,
    local_sem,
    send_sem,
    recv_sem,
):
    f32, bf16 = jnp.float32, jnp.bfloat16
    s = lax.axis_index("sp")
    t = lax.axis_index("tp")
    z, x = s // X, s % X
    parity = z % 2
    other = 1 - parity
    zpair = z + 1 - 2 * parity
    spair = zpair * X + x
    tokens = q_one.shape[0]
    piece = tokens // T
    kw = k_one.shape[1] // 2
    vw = values.shape[1] // 2
    group = X * down_weight.shape[0]
    groups = Z // 2

    def at_z(d):
        return (z + d) % Z

    def from_z(d):
        return (z - d + Z) % Z

    def at_x(d):
        return (x + d) % X

    def from_x(d):
        return (x - d + X) % X

    def at_t(d):
        return (t + d) % T

    def from_t(d):
        return (t - d + T) % T

    barrier = pltpu.get_barrier_semaphore()
    peers = [(at_z(d) * X + x, t) for d in range(1, Z)]
    peers += [(z * X + at_x(d), t) for d in range(1, X)]
    peers += [(s, at_t(d)) for d in range(1, T)]
    peers += [(spair, at_t(d)) for d in range(1, T)]
    for sp_at, tp_at in peers:
        pl.semaphore_signal(
            barrier, inc=1, device_id={"sp": sp_at, "tp": tp_at},
            device_id_type=pl.DeviceIdType.MESH,
        )

    def columns(ref, half, size):
        return ref.at[:, pl.ds(pl.multiple_of(half * size, size), size)]

    moves = [
        (columns(q_one, other, kw), queries_out.at[0]),
        (columns(q_two, other, kw), queries_out.at[1]),
        (columns(k_one, other, kw), kv_out.at[:, pl.ds(0, kw)]),
        (columns(k_two, other, kw), kv_out.at[:, pl.ds(kw, kw)]),
        (columns(values, other, vw), kv_out.at[:, pl.ds(2 * kw, vw)]),
        (columns(k_one, parity, kw), kv.at[s, :, pl.ds(0, kw)]),
        (columns(k_two, parity, kw), kv.at[s, :, pl.ds(kw, kw)]),
        (columns(values, parity, vw), kv.at[s, :, pl.ds(2 * kw, vw)]),
        (columns(q_one, parity, kw), queries.at[0, 0]),
        (columns(q_two, parity, kw), queries.at[0, 1]),
        (out_weight, outw.at[z // 2, x]),
        (down_weight, downw.at[z // 2, x]),
        (gate_weight, gate),
        (up_weight, up),
    ]
    moving = [
        pltpu.make_async_copy(src, dst, local_sem.at[i]) for i, (src, dst) in enumerate(moves)
    ]
    for copy in moving:
        copy.start()

    names = {}
    sent = []

    def slot(name):
        return names.setdefault(name, len(names))

    def send(src, dst, name, sp_at, tp_at):
        k = slot(name)
        copy = pltpu.make_async_remote_copy(
            src_ref=src, dst_ref=dst, send_sem=send_sem.at[k], recv_sem=recv_sem.at[k],
            device_id={"sp": sp_at, "tp": tp_at}, device_id_type=pl.DeviceIdType.MESH,
        )
        copy.start()
        sent.append(copy)

    def arrive(ref, name):
        k = slot(name)
        pltpu.make_async_remote_copy(
            src_ref=ref, dst_ref=ref, send_sem=send_sem.at[k], recv_sem=recv_sem.at[k],
            device_id={"sp": s, "tp": t}, device_id_type=pl.DeviceIdType.MESH,
        ).wait_recv()

    def kv_at(zz, xx):
        return kv.at[zz * X + xx]

    def out_at(zz, xx):
        return outw.at[zz // 2, xx]

    rows_chunk = down_weight.shape[0] // C

    def down_at(c):
        return lambda zz, xx: downw.at[zz // 2, xx, pl.ds(c * rows_chunk, rows_chunk)]

    def send_z(kind, ref, d):
        send(ref(z, x), ref(z, x), (kind, "z", d), at_z(d) * X + x, t)

    def wait_z(kind, ref, d):
        arrive(ref(from_z(d), x), (kind, "z", d))

    def forward_x(kind, ref, d):
        for dx in range(1, X):
            block = ref(from_z(d), x)
            send(block, block, (kind, "x", d, dx), z * X + at_x(dx), t)

    def wait_x(kind, ref, d):
        for dx in range(1, X):
            arrive(ref(from_z(d), from_x(dx)), (kind, "x", d, dx))

    def down_z(c):
        for d in range(2, Z, 2):
            send_z("down%d" % c, down_at(c), d)

    def down_own(c):
        forward_x("down%d" % c, down_at(c), 0)

    def down_forward(c):
        for d in range(2, Z, 2):
            wait_z("down%d" % c, down_at(c), d)
            forward_x("down%d" % c, down_at(c), d)

    for copy in moving[:8]:
        copy.wait()
    pl.semaphore_wait(barrier, len(peers))
    for d in range(1, Z):
        send(
            kv_out if d % 2 else kv.at[s], kv.at[s], ("kv", "z", d), at_z(d) * X + x, t
        )
        if d == 1:
            forward_x("kv", kv_at, 0)
            send(queries_out, queries.at[1], ("query",), spair, t)
    for copy in moving[8:12]:
        copy.wait()
    for d in range(2, Z, 2):
        send_z("out", out_at, d)
    down_z(0)
    for d in range(1, Z):
        wait_z("kv", kv_at, d)
        forward_x("kv", kv_at, d)
    forward_x("out", out_at, 0)
    down_own(0)
    arrive(queries.at[1], ("query",))
    for d in range(Z):
        wait_x("kv", kv_at, d)

    half_heads = heads // 2
    head_size = kw // half_heads
    value_size = vw // half_heads
    per = min(half_heads, 128 // head_size)
    scale = head_size ** (-0.5)
    source_count = kv.shape[0]
    block_count = max(1, (source_count * tokens) // 1024)
    block_sources = source_count // block_count
    block_keys = block_sources * tokens
    lanes = lax.broadcasted_iota(jnp.int32, (1, per * head_size), 1) // head_size

    def map_outputs(which, index, first):
        width = per * head_size
        q = queries[which, index, :, first * head_size : first * head_size + width]
        stacked = jnp.concatenate(
            [jnp.where(lanes == i, q, jnp.zeros_like(q)) for i in range(per)], axis=0
        )
        base = index * kw + first * head_size

        def block(b, state):
            rows = pl.ds(b * block_sources, block_sources)
            keys = kv[rows, :, base : base + width]
            scores = lax.dot_general(
                stacked, keys.reshape(block_keys, width), ROWS_ROWS, preferred_element_type=f32
            ) * scale
            newest = jnp.max(scores, axis=1, keepdims=True)
            if state is not None:
                newest = jnp.maximum(newest, state[0])
            shifted = jnp.exp(scores - newest)
            totals = jnp.sum(shifted, axis=1, keepdims=True)
            rounded = shifted.astype(bf16)
            products = []
            for i in range(per):
                start = 2 * kw + (first + i) * value_size
                v = kv[rows, :, start : start + value_size].reshape(block_keys, value_size)
                products.append(
                    jnp.dot(
                        rounded[i * tokens : (i + 1) * tokens], v, preferred_element_type=f32
                    )
                )
            product = jnp.concatenate(products, axis=0)
            if state is not None:
                factor = jnp.exp(state[0] - newest)
                totals = totals + state[1] * factor
                product = product + state[2] * factor
            return newest, totals, product

        if block_count == 1:
            state = block(0, None)
        else:
            state = lax.fori_loop(
                0,
                block_count,
                block,
                (
                    jnp.full((per * tokens, 1), -jnp.inf, f32),
                    jnp.zeros((per * tokens, 1), f32),
                    jnp.zeros((per * tokens, value_size), f32),
                ),
            )
        return state[2] / state[1]

    for which in (1, 0):
        for first in range(0, half_heads, per):
            one = map_outputs(which, 0, first)
            two = map_outputs(which, 1, first)
            for i in range(per):
                rows = slice(i * tokens, (i + 1) * tokens)
                difference = one[rows] - lam[parity * half_heads + first + i] * two[rows]
                scaled = difference * lax.rsqrt(
                    jnp.mean(difference * difference, axis=1, keepdims=True) + epsilon
                )
                start = (first + i) * value_size
                attended[which, parity, :, start : start + value_size] = (
                    scaled * head_gain[...]
                ).astype(bf16)
        send(
            attended.at[which, parity], attended.at[1 - which, parity], ("att", which), spair, t
        )

    for d in range(2, Z, 2):
        wait_z("out", out_at, d)
        forward_x("out", out_at, d)
    for c in range(1, C):
        if c == 1:
            down_z(c)
        down_own(c)
    for d in range(0, Z, 2):
        wait_x("out", out_at, d)
    for which in (1, 0):
        arrive(attended.at[1 - which, other], ("att", which))

    def spread(kind, which, g, product, part, rec):
        cols = slice(g * group, (g + 1) * group)
        part[which, :, :, cols] = product.astype(bf16).reshape(T, piece, group)
        for d in range(0 if which else 1, T):
            send(
                part.at[which, at_t(d), :, pl.ds(g * group, group)],
                rec.at[parity, t, :, pl.ds(g * group, group)],
                (kind, which, g, d), spair if which else s, at_t(d),
            )

    def collect(kind, base, part, rec, put):
        rec[parity, t] = part[0, t]
        for g in range(groups):
            for d in range(1, T):
                arrive(
                    rec.at[parity, from_t(d), :, pl.ds(g * group, group)], (kind, 0, g, d)
                )
            for d in range(T):
                arrive(
                    rec.at[1 - parity, from_t(d), :, pl.ds(g * group, group)], (kind, 1, g, d)
                )
            for side in range(2):
                start = (2 * g + side) * group
                total = rec[side, 0, :, g * group : (g + 1) * group].astype(f32)
                for i in range(1, T):
                    total = total + rec[side, i, :, g * group : (g + 1) * group].astype(f32)
                put(start, base[:, start : start + group].astype(f32) + total)

    for g in range(groups):
        weight = outw[g].reshape(group, 2 * vw)
        both = [attended[:, h].reshape(2 * tokens, vw) for h in range(2)]
        product = lax.dot_general(
            both[0], weight[:, :vw], ROWS_ROWS, preferred_element_type=f32
        ) + lax.dot_general(both[1], weight[:, vw:], ROWS_ROWS, preferred_element_type=f32)
        for which in (1, 0):
            spread(
                "one", which, g, product[which * tokens : (which + 1) * tokens], part_one, rec_one
            )
    if C > 2:
        down_z(2)
    down_forward(0)

    def put_after(start, block):
        after[:, start : start + group] = block.astype(bf16).astype(f32)

    collect("one", residual, part_one, rec_one, put_after)
    stream = after[...]
    scaled = stream * lax.rsqrt(jnp.mean(stream * stream, axis=1, keepdims=True) + epsilon)
    normed[t] = (scaled * norm_gain[...]).astype(bf16)
    for d in range(1, T):
        send(normed.at[t], normed.at[t], ("norm", d), s, at_t(d))
    for c in range(3, C):
        down_z(c)
    if C > 1:
        down_forward(1)
    for copy in moving[12:]:
        copy.wait()
    for d in range(1, T):
        arrive(normed.at[from_t(d)], ("norm", d))

    width = hidden.shape[2]
    spans = [(c, min(512, width - c)) for c in range(0, width, 512)]
    rows_in = normed[...].reshape(tokens, normed.shape[2])
    for c, n in spans:
        gate_part = jnp.dot(rows_in, gate[:, c : c + n], preferred_element_type=f32)
        up_part = jnp.dot(rows_in, up[:, c : c + n], preferred_element_type=f32)
        hidden[0, :, c : c + n] = (
            gate_part / (1.0 + jnp.exp(-gate_part)) * up_part
        ).astype(bf16)
        send(hidden.at[0, :, pl.ds(c, n)], hidden.at[1, :, pl.ds(c, n)], ("hid", c), spair, t)
    for c in range(2, C):
        down_forward(c)
    for c in range(C):
        for d in range(0, Z, 2):
            wait_x("down%d" % c, down_at(c), d)
    for which in range(2):
        if which:
            for c, n in spans:
                arrive(hidden.at[1, :, pl.ds(c, n)], ("hid", c))
        for g in range(groups):
            product = lax.dot_general(
                hidden[which], downw[g].reshape(group, width), ROWS_ROWS,
                preferred_element_type=f32,
            )
            spread("two", which, g, product, part_two, rec_two)

    def put_result(start, block):
        result[:, start : start + group] = block.astype(bf16)

    collect("two", after, part_two, rec_two, put_result)
    for copy in sent:
        copy.wait_send()


def local(Z, X, T, *arrays):
    (residual, q_one, k_one, q_two, k_two, values, lam, head_gain, out_weight, norm_gain,
     gate_weight, up_weight, down_weight) = arrays
    sp = Z * X
    bf16 = jnp.bfloat16
    tokens, kw = k_one.shape
    vw = values.shape[1]
    piece, model = residual.shape
    width = gate_weight.shape[1]
    rows_down = down_weight.shape[0]
    C = max(1, min(4, rows_down // 32))
    half = model // 2
    vmem = pl.BlockSpec(memory_space=pltpu.VMEM)
    anywhere = pl.BlockSpec(memory_space=pl.ANY)
    smem = pl.BlockSpec(memory_space=pltpu.SMEM)
    semaphores = Z + Z * X + (1 + C) * (Z // 2) * (1 + X) + 8 * T * Z + 64
    return pl.pallas_call(
        functools.partial(kernel, Z, X, T, C, lam.shape[0]),
        out_shape=jax.ShapeDtypeStruct((piece, model), bf16),
        in_specs=[
            vmem, anywhere, anywhere, anywhere, anywhere, anywhere, smem, vmem, anywhere, vmem,
            anywhere, anywhere, anywhere,
        ],
        out_specs=vmem,
        scratch_shapes=[
            pltpu.VMEM((2, 2, tokens, kw // 2), bf16),
            pltpu.VMEM((2, tokens, kw // 2), bf16),
            pltpu.VMEM((sp, tokens, kw + vw // 2), bf16),
            pltpu.VMEM((tokens, kw + vw // 2), bf16),
            pltpu.VMEM((Z // 2, X, out_weight.shape[0], vw), bf16),
            pltpu.VMEM((Z // 2, X, rows_down, width), bf16),
            pltpu.VMEM(gate_weight.shape, bf16),
            pltpu.VMEM(up_weight.shape, bf16),
            pltpu.VMEM((2, 2, tokens, vw // 2), bf16),
            pltpu.VMEM((2, T, piece, half), bf16),
            pltpu.VMEM((2, T, piece, half), bf16),
            pltpu.VMEM((piece, model), jnp.float32),
            pltpu.VMEM((T, piece, model), bf16),
            pltpu.VMEM((2, tokens, width), bf16),
            pltpu.VMEM((2, T, piece, half), bf16),
            pltpu.VMEM((2, T, piece, half), bf16),
            pltpu.SemaphoreType.DMA((14,)),
            pltpu.SemaphoreType.DMA((semaphores,)),
            pltpu.SemaphoreType.DMA((semaphores,)),
        ],
        compiler_params=pltpu.CompilerParams(
            collective_id=0, has_side_effects=True, vmem_limit_bytes=60 * 1024 * 1024
        ),
    )(
        residual, q_one, k_one, q_two, k_two, values, lam, head_gain.reshape(1, -1), out_weight,
        norm_gain.reshape(1, -1), gate_weight, up_weight, down_weight,
    )


def solution(mesh):
    Z, X = split_sp(mesh.shape["sp"])
    return jax.shard_map(
        functools.partial(local, Z, X, mesh.shape["tp"]),
        mesh=mesh,
        in_specs=(
            P(("sp", "tp"), None),
            P("sp", "tp"),
            P("sp", "tp"),
            P("sp", "tp"),
            P("sp", "tp"),
            P("sp", "tp"),
            P("tp"),
            P(),
            P("sp", "tp"),
            P(),
            P(None, "tp"),
            P(None, "tp"),
            P("sp", "tp"),
        ),
        out_specs=P(("sp", "tp"), None),
        check_vma=False,
    )
```

```python
import functools

import jax
import jax.numpy as jnp
from jax import lax
from jax.experimental import pallas as pl
from jax.experimental.pallas import tpu as pltpu
from jax.sharding import PartitionSpec as P

epsilon = 1e-06
ROWS_ROWS = (((1,), (1,)), ((), ()))
CHUNKS = 8
STARTS = (0, 3, 6, 8)
FORWARDS = (2, 4, 8)


def split_sp(size):
    inner = 1
    while (2 * inner) * (2 * inner) <= size:
        inner *= 2
    return size // inner, inner


def kernel(
    Z,
    X,
    T,
    C,
    heads,
    residual,
    q_one,
    k_one,
    q_two,
    k_two,
    values,
    lam,
    head_gain,
    out_weight,
    norm_gain,
    gate_weight,
    up_weight,
    down_weight,
    result,
    queries,
    queries_out,
    kv,
    kv_out,
    outw,
    downw,
    gate,
    up,
    attended,
    part_one,
    rec_one,
    after,
    normed,
    hidden,
    part_two,
    rec_two,
    local_sem,
    send_sem,
    recv_sem,
):
    f32, bf16 = jnp.float32, jnp.bfloat16
    s = lax.axis_index("sp")
    t = lax.axis_index("tp")
    z, x = s // X, s % X
    parity = z % 2
    other = 1 - parity
    zpair = z + 1 - 2 * parity
    spair = zpair * X + x
    tokens = q_one.shape[0]
    piece = tokens // T
    kw = k_one.shape[1] // 2
    vw = values.shape[1] // 2
    group = X * down_weight.shape[0]
    groups = Z // 2

    def at_z(d):
        return (z + d) % Z

    def from_z(d):
        return (z - d + Z) % Z

    def at_x(d):
        return (x + d) % X

    def from_x(d):
        return (x - d + X) % X

    def at_t(d):
        return (t + d) % T

    def from_t(d):
        return (t - d + T) % T

    barrier = pltpu.get_barrier_semaphore()
    peers = [(at_z(d) * X + x, t) for d in range(1, Z)]
    peers += [(z * X + at_x(d), t) for d in range(1, X)]
    peers += [(s, at_t(d)) for d in range(1, T)]
    peers += [(spair, at_t(d)) for d in range(1, T)]
    for sp_at, tp_at in peers:
        pl.semaphore_signal(
            barrier, inc=1, device_id={"sp": sp_at, "tp": tp_at},
            device_id_type=pl.DeviceIdType.MESH,
        )

    def columns(ref, half, size):
        return ref.at[:, pl.ds(pl.multiple_of(half * size, size), size)]

    moves = [
        (columns(q_one, other, kw), queries_out.at[0]),
        (columns(q_two, other, kw), queries_out.at[1]),
        (columns(k_one, other, kw), kv_out.at[:, pl.ds(0, kw)]),
        (columns(k_two, other, kw), kv_out.at[:, pl.ds(kw, kw)]),
        (columns(values, other, vw), kv_out.at[:, pl.ds(2 * kw, vw)]),
        (columns(k_one, parity, kw), kv.at[s, :, pl.ds(0, kw)]),
        (columns(k_two, parity, kw), kv.at[s, :, pl.ds(kw, kw)]),
        (columns(values, parity, vw), kv.at[s, :, pl.ds(2 * kw, vw)]),
        (columns(q_one, parity, kw), queries.at[0, 0]),
        (columns(q_two, parity, kw), queries.at[0, 1]),
        (out_weight, outw.at[z // 2, x]),
        (down_weight, downw.at[z // 2, x]),
        (gate_weight, gate),
        (up_weight, up),
    ]
    moving = [
        pltpu.make_async_copy(src, dst, local_sem.at[i]) for i, (src, dst) in enumerate(moves)
    ]
    for copy in moving:
        copy.start()

    names = {}
    sent = []

    def slot(name):
        return names.setdefault(name, len(names))

    def send(src, dst, name, sp_at, tp_at):
        k = slot(name)
        copy = pltpu.make_async_remote_copy(
            src_ref=src, dst_ref=dst, send_sem=send_sem.at[k], recv_sem=recv_sem.at[k],
            device_id={"sp": sp_at, "tp": tp_at}, device_id_type=pl.DeviceIdType.MESH,
        )
        copy.start()
        sent.append(copy)

    def arrive(ref, name):
        k = slot(name)
        pltpu.make_async_remote_copy(
            src_ref=ref, dst_ref=ref, send_sem=send_sem.at[k], recv_sem=recv_sem.at[k],
            device_id={"sp": s, "tp": t}, device_id_type=pl.DeviceIdType.MESH,
        ).wait_recv()

    def kv_at(lo, hi):
        return lambda zz, xx: kv.at[zz * X + xx, :, pl.ds(lo, hi - lo)]

    parts = [
        (kind, kv_at(lo, hi), lo, hi)
        for kind, lo, hi in (("kvk", 0, 2 * kw), ("kvv", 2 * kw, 2 * kw + vw))
    ]

    def out_at(zz, xx):
        return outw.at[zz // 2, xx]

    rows_chunk = down_weight.shape[0] // C

    def down_at(c):
        return lambda zz, xx: downw.at[zz // 2, xx, pl.ds(c * rows_chunk, rows_chunk)]

    def send_z(kind, ref, d):
        send(ref(z, x), ref(z, x), (kind, "z", d), at_z(d) * X + x, t)

    def wait_z(kind, ref, d):
        arrive(ref(from_z(d), x), (kind, "z", d))

    def forward_x(kind, ref, d):
        for dx in range(1, X):
            block = ref(from_z(d), x)
            send(block, block, (kind, "x", d, dx), z * X + at_x(dx), t)

    def wait_x(kind, ref, d):
        for dx in range(1, X):
            arrive(ref(from_z(d), from_x(dx)), (kind, "x", d, dx))

    def down_z(c):
        for d in range(2, Z, 2):
            send_z("down%d" % c, down_at(c), d)

    def down_own(c):
        forward_x("down%d" % c, down_at(c), 0)

    def down_forward(c):
        for d in range(2, Z, 2):
            wait_z("down%d" % c, down_at(c), d)
            forward_x("down%d" % c, down_at(c), d)

    for copy in moving[:8]:
        copy.wait()
    pl.semaphore_wait(barrier, len(peers))
    for kind, ref, lo, hi in parts:
        cols = pl.ds(lo, hi - lo)
        for d in range(1, Z):
            source = kv_out.at[:, cols] if d % 2 else kv.at[s, :, cols]
            send(source, kv.at[s, :, cols], (kind, "z", d), at_z(d) * X + x, t)
        forward_x(kind, ref, 0)
        if lo == 0:
            send(queries_out, queries.at[1], ("query",), spair, t)
    for copy in moving[8:12]:
        copy.wait()
    for d in range(2, Z, 2):
        send_z("out", out_at, d)
    starts = [min(C, k * C // CHUNKS) for k in STARTS]
    forwards = [min(C, k * C // CHUNKS) for k in FORWARDS]
    for c in range(starts[0]):
        down_z(c)
    for kind, ref, lo, hi in parts:
        for d in range(1, Z):
            wait_z(kind, ref, d)
            forward_x(kind, ref, d)
    forward_x("out", out_at, 0)
    for c in range(starts[0]):
        down_own(c)
    arrive(queries.at[1], ("query",))
    for kind, ref, lo, hi in parts:
        for d in range(Z):
            wait_x(kind, ref, d)

    half_heads = heads // 2
    head_size = kw // half_heads
    value_size = vw // half_heads
    per = min(half_heads, 128 // head_size)
    scale = head_size ** (-0.5)
    source_count = kv.shape[0]
    block_count = max(1, (source_count * tokens) // 1024)
    block_sources = source_count // block_count
    block_keys = block_sources * tokens
    lanes = lax.broadcasted_iota(jnp.int32, (1, per * head_size), 1) // head_size

    def map_outputs(which, index, first):
        width = per * head_size
        q = queries[which, index, :, first * head_size : first * head_size + width]
        stacked = jnp.concatenate(
            [jnp.where(lanes == i, q, jnp.zeros_like(q)) for i in range(per)], axis=0
        )
        base = index * kw + first * head_size

        def block(b, state):
            rows = pl.ds(b * block_sources, block_sources)
            keys = kv[rows, :, base : base + width]
            scores = lax.dot_general(
                stacked, keys.reshape(block_keys, width), ROWS_ROWS, preferred_element_type=f32
            ) * scale
            newest = jnp.max(scores, axis=1, keepdims=True)
            if state is not None:
                newest = jnp.maximum(newest, state[0])
            shifted = jnp.exp(scores - newest)
            totals = jnp.sum(shifted, axis=1, keepdims=True)
            rounded = shifted.astype(bf16)
            products = []
            for i in range(per):
                start = 2 * kw + (first + i) * value_size
                v = kv[rows, :, start : start + value_size].reshape(block_keys, value_size)
                products.append(
                    jnp.dot(
                        rounded[i * tokens : (i + 1) * tokens], v, preferred_element_type=f32
                    )
                )
            product = jnp.concatenate(products, axis=0)
            if state is not None:
                factor = jnp.exp(state[0] - newest)
                totals = totals + state[1] * factor
                product = product + state[2] * factor
            return newest, totals, product

        if block_count == 1:
            state = block(0, None)
        else:
            state = lax.fori_loop(
                0,
                block_count,
                block,
                (
                    jnp.full((per * tokens, 1), -jnp.inf, f32),
                    jnp.zeros((per * tokens, 1), f32),
                    jnp.zeros((per * tokens, value_size), f32),
                ),
            )
        return state[2] / state[1]

    for which in (1, 0):
        for first in range(0, half_heads, per):
            one = map_outputs(which, 0, first)
            two = map_outputs(which, 1, first)
            for i in range(per):
                rows = slice(i * tokens, (i + 1) * tokens)
                difference = one[rows] - lam[parity * half_heads + first + i] * two[rows]
                scaled = difference * lax.rsqrt(
                    jnp.mean(difference * difference, axis=1, keepdims=True) + epsilon
                )
                start = (first + i) * value_size
                attended[which, parity, :, start : start + value_size] = (
                    scaled * head_gain[...]
                ).astype(bf16)
        send(
            attended.at[which, parity], attended.at[1 - which, parity], ("att", which), spair, t
        )

    for d in range(2, Z, 2):
        wait_z("out", out_at, d)
        forward_x("out", out_at, d)
    for c in range(starts[0], starts[1]):
        down_z(c)
    for c in range(starts[0], C):
        down_own(c)
    for d in range(0, Z, 2):
        wait_x("out", out_at, d)
    for which in (1, 0):
        arrive(attended.at[1 - which, other], ("att", which))

    def spread(kind, which, g, product, part, rec):
        cols = slice(g * group, (g + 1) * group)
        part[which, :, :, cols] = product.astype(bf16).reshape(T, piece, group)
        for d in range(0 if which else 1, T):
            send(
                part.at[which, at_t(d), :, pl.ds(g * group, group)],
                rec.at[parity, t, :, pl.ds(g * group, group)],
                (kind, which, g, d), spair if which else s, at_t(d),
            )

    def collect(kind, base, part, rec, put):
        rec[parity, t] = part[0, t]
        for g in range(groups):
            for d in range(1, T):
                arrive(
                    rec.at[parity, from_t(d), :, pl.ds(g * group, group)], (kind, 0, g, d)
                )
            for d in range(T):
                arrive(
                    rec.at[1 - parity, from_t(d), :, pl.ds(g * group, group)], (kind, 1, g, d)
                )
            for side in range(2):
                start = (2 * g + side) * group
                total = rec[side, 0, :, g * group : (g + 1) * group].astype(f32)
                for i in range(1, T):
                    total = total + rec[side, i, :, g * group : (g + 1) * group].astype(f32)
                put(start, base[:, start : start + group].astype(f32) + total)

    for g in range(groups):
        weight = outw[g].reshape(group, 2 * vw)
        both = [attended[:, h].reshape(2 * tokens, vw) for h in range(2)]
        product = lax.dot_general(
            both[0], weight[:, :vw], ROWS_ROWS, preferred_element_type=f32
        ) + lax.dot_general(both[1], weight[:, vw:], ROWS_ROWS, preferred_element_type=f32)
        for which in (1, 0):
            spread(
                "one", which, g, product[which * tokens : (which + 1) * tokens], part_one, rec_one
            )
    for c in range(starts[1], starts[2]):
        down_z(c)
    for c in range(forwards[0]):
        down_forward(c)

    def put_after(start, block):
        after[:, start : start + group] = block.astype(bf16).astype(f32)

    collect("one", residual, part_one, rec_one, put_after)
    stream = after[...]
    scaled = stream * lax.rsqrt(jnp.mean(stream * stream, axis=1, keepdims=True) + epsilon)
    normed[t] = (scaled * norm_gain[...]).astype(bf16)
    for d in range(1, T):
        send(normed.at[t], normed.at[t], ("norm", d), s, at_t(d))
    for c in range(starts[2], C):
        down_z(c)
    for c in range(forwards[0], forwards[1]):
        down_forward(c)
    for copy in moving[12:]:
        copy.wait()
    for d in range(1, T):
        arrive(normed.at[from_t(d)], ("norm", d))

    width = hidden.shape[2]
    spans = [(c, min(512, width - c)) for c in range(0, width, 512)]
    rows_in = normed[...].reshape(tokens, normed.shape[2])
    for c, n in spans:
        gate_part = jnp.dot(rows_in, gate[:, c : c + n], preferred_element_type=f32)
        up_part = jnp.dot(rows_in, up[:, c : c + n], preferred_element_type=f32)
        hidden[0, :, c : c + n] = (
            gate_part / (1.0 + jnp.exp(-gate_part)) * up_part
        ).astype(bf16)
        send(hidden.at[0, :, pl.ds(c, n)], hidden.at[1, :, pl.ds(c, n)], ("hid", c), spair, t)
    for c in range(forwards[1], C):
        down_forward(c)
    for c in range(C):
        for d in range(0, Z, 2):
            wait_x("down%d" % c, down_at(c), d)
    for which in range(2):
        if which:
            for c, n in spans:
                arrive(hidden.at[1, :, pl.ds(c, n)], ("hid", c))
        for g in range(groups):
            product = lax.dot_general(
                hidden[which], downw[g].reshape(group, width), ROWS_ROWS,
                preferred_element_type=f32,
            )
            spread("two", which, g, product, part_two, rec_two)

    def put_result(start, block):
        result[:, start : start + group] = block.astype(bf16)

    collect("two", after, part_two, rec_two, put_result)
    for copy in sent:
        copy.wait_send()


def local(Z, X, T, *arrays):
    (residual, q_one, k_one, q_two, k_two, values, lam, head_gain, out_weight, norm_gain,
     gate_weight, up_weight, down_weight) = arrays
    sp = Z * X
    bf16 = jnp.bfloat16
    tokens, kw = k_one.shape
    vw = values.shape[1]
    piece, model = residual.shape
    width = gate_weight.shape[1]
    rows_down = down_weight.shape[0]
    C = max(1, min(CHUNKS, rows_down // 32))
    half = model // 2
    vmem = pl.BlockSpec(memory_space=pltpu.VMEM)
    anywhere = pl.BlockSpec(memory_space=pl.ANY)
    smem = pl.BlockSpec(memory_space=pltpu.SMEM)
    semaphores = 2 * (Z + Z * X) + (1 + C) * (Z // 2) * (1 + X) + 8 * T * Z + 64
    return pl.pallas_call(
        functools.partial(kernel, Z, X, T, C, lam.shape[0]),
        out_shape=jax.ShapeDtypeStruct((piece, model), bf16),
        in_specs=[
            vmem, anywhere, anywhere, anywhere, anywhere, anywhere, smem, vmem, anywhere, vmem,
            anywhere, anywhere, anywhere,
        ],
        out_specs=vmem,
        scratch_shapes=[
            pltpu.VMEM((2, 2, tokens, kw // 2), bf16),
            pltpu.VMEM((2, tokens, kw // 2), bf16),
            pltpu.VMEM((sp, tokens, kw + vw // 2), bf16),
            pltpu.VMEM((tokens, kw + vw // 2), bf16),
            pltpu.VMEM((Z // 2, X, out_weight.shape[0], vw), bf16),
            pltpu.VMEM((Z // 2, X, rows_down, width), bf16),
            pltpu.VMEM(gate_weight.shape, bf16),
            pltpu.VMEM(up_weight.shape, bf16),
            pltpu.VMEM((2, 2, tokens, vw // 2), bf16),
            pltpu.VMEM((2, T, piece, half), bf16),
            pltpu.VMEM((2, T, piece, half), bf16),
            pltpu.VMEM((piece, model), jnp.float32),
            pltpu.VMEM((T, piece, model), bf16),
            pltpu.VMEM((2, tokens, width), bf16),
            pltpu.VMEM((2, T, piece, half), bf16),
            pltpu.VMEM((2, T, piece, half), bf16),
            pltpu.SemaphoreType.DMA((14,)),
            pltpu.SemaphoreType.DMA((semaphores,)),
            pltpu.SemaphoreType.DMA((semaphores,)),
        ],
        compiler_params=pltpu.CompilerParams(
            collective_id=0, has_side_effects=True, vmem_limit_bytes=60 * 1024 * 1024
        ),
    )(
        residual, q_one, k_one, q_two, k_two, values, lam, head_gain.reshape(1, -1), out_weight,
        norm_gain.reshape(1, -1), gate_weight, up_weight, down_weight,
    )


def solution(mesh):
    Z, X = split_sp(mesh.shape["sp"])
    return jax.shard_map(
        functools.partial(local, Z, X, mesh.shape["tp"]),
        mesh=mesh,
        in_specs=(
            P(("sp", "tp"), None),
            P("sp", "tp"),
            P("sp", "tp"),
            P("sp", "tp"),
            P("sp", "tp"),
            P("sp", "tp"),
            P("tp"),
            P(),
            P("sp", "tp"),
            P(),
            P(None, "tp"),
            P(None, "tp"),
            P("sp", "tp"),
        ),
        out_specs=P(("sp", "tp"), None),
        check_vma=False,
    )
```
